32 devices in a mesh: grp: 2 (over y), sp: 4 (over z), tp: 4 (over x, core).
Axes of the slice: x: 2, y: 2, z: 4, core: 2. Of those that a mesh axis runs over, the one named last changes fastest.
Arguments:
- queries: bfloat16 [4096, 1024], P(('grp', 'sp'), 'tp'), parts along dimension 0, may hold values from -6 to 6
- keys: bfloat16 [4096, 1024], P(('grp', 'sp'), 'tp'), parts along dimension 0, may hold values from -6 to 6
- values: bfloat16 [4096, 2048], P(('grp', 'sp'), 'tp'), parts along dimension 0, may hold values from -6 to 6
- in_gate: float32 [8, 4096], P('tp', ('grp', 'sp')), parts along dimension 1, may hold values from -4 to 220
- forget_gate: float32 [8, 4096], P('tp', ('grp', 'sp')), parts along dimension 1, may hold values from 0 to 16
- head_gain: float32 [2048], P('tp'), may hold values from 0.1 to 1.9
- out_weight: bfloat16 [2048, 2048], P('tp'), may hold values from -0.125 to 0.125
- resid: bfloat16 [4096, 2048], P(('grp', 'sp', 'tp')), parts along dimension 0, may hold values from -6 to 6
- norm_gain: float32 [2048], replicated, may hold values from 0.1 to 1.9
- expert_ids: int32 [4096, 2], P(('grp', 'sp', 'tp')), parts along dimension 0, may hold values from 0 to 15, all different within a row; in each aligned block of 128 rows (0 to 127, 128 to 255, ...) at most 64 rows name the same one
- expert_mix: float32 [4096, 2], P(('grp', 'sp', 'tp')), parts along dimension 0, may hold values from 0.25 to 1
- gate_weight: bfloat16 [16, 2048, 512], P(('sp', 'tp')), may hold values from -0.125 to 0.125
- up_weight: bfloat16 [16, 2048, 512], P(('sp', 'tp')), may hold values from -0.125 to 0.125
- down_weight: bfloat16 [16, 512, 2048], P(('sp', 'tp')), may hold values from -0.25 to 0.25
Outputs:
- final: bfloat16 [4096, 2048], P(('grp', 'sp', 'tp')), parts along dimension 0
The draws below stay inside these ranges and needn't reach their ends.
There are 2 independent parts, one for each index of `grp`. The reference program is written for one: setup_inputs(seed, part) draws one part's arguments, and reference() takes and returns one part's arrays. A program takes and returns all parts, laid end to end along the dimension named above; an argument that names none is the same for every part. Nothing has to cross between parts.
Inputs may be any that keep to these rules, and one draw needn't show every extreme that they name: `expert_ids`: each row names 2 different experts. In each aligned block of 128 rows (the rows of one device) no expert is named more than 64 times, a bound that some block reaches.
All inputs are finite; a program needn't handle non-finite values.
Results may differ from the reference program's by a relative error of at most 0.013.
Values may be sent and summed in bfloat16 or wider, within the bound.
A program may use at most 128 MiB of HBM per device.

```python
import math
import jax
import jax.numpy as jnp
import numpy as np
from jax import lax

D = 2048
HEADS = 8
QK_HEAD = 128
V_HEAD = 256
FF = 512
BLOCK = 128
TOPK = 2
TOK_DEV = 512
TOKENS = 2048
TOK_SHARD = 128
EXPERTS = 16
CAP = 64
N_TP = 4


def draw_in_gate(key, part):
    base_key = jax.random.fold_in(key, 0)
    sample = jnp.clip(jax.random.normal(base_key, (HEADS, TOKENS), jnp.float32), -4.0, 4.0)
    return sample


def draw_forget_gate(key, part):
    order_key, region_key, block_key, noise_key = jax.random.split(key, 4)
    ranks = jax.random.permutation(order_key, HEADS)
    slow = ranks < HEADS // 2
    base = jnp.where(slow, jnp.log(TOKENS / 1.2), jnp.log(40.0)).astype(jnp.float32)
    regions = jax.random.uniform(region_key, (HEADS, TOKENS // TOK_DEV, 1), jnp.float32, -0.8, 0.8)
    regions = jnp.broadcast_to(regions, (HEADS, TOKENS // TOK_DEV, TOK_DEV)).reshape(HEADS, TOKENS)
    blocks = jax.random.uniform(block_key, (HEADS, TOKENS // BLOCK, 1), jnp.float32, -0.3, 0.3)
    blocks = jnp.broadcast_to(blocks, (HEADS, TOKENS // BLOCK, BLOCK)).reshape(HEADS, TOKENS)
    noise = jnp.clip(0.5 * jax.random.normal(noise_key, (HEADS, TOKENS), jnp.float32), -1.5, 1.5)
    return base[:, None] + regions + blocks + noise


def levels(key, shape, pieces, least, largest):
    level, own = 1.0, jax.random.fold_in(key, 6)
    for position, parts in pieces:
        steps = jnp.exp(jax.random.uniform(jax.random.fold_in(own, position), (parts,), jnp.float32, least / len(pieces), largest / len(pieces)))
        level = level * jnp.repeat(steps, shape[position] // parts).reshape([-1 if axis == position else 1 for axis in range(len(shape))])
    return level


def routed_block(stream_key, own, number, rows, number_of, top, reach, slope):
    ranking = jax.random.permutation(stream_key, number_of)
    crowded, common = load_shares(number_of, rows * top, reach, slope, True), load_shares(number_of, rows * top, reach, slope, False)
    places = jnp.arange(number_of)

    def named(tallies, rotation):
        used = int((tallies > 0).sum())
        fixed = max(1, used // 4)
        passed = fixed + (places - fixed + rotation * (used - fixed)) % max(1, number_of - fixed)
        return jnp.zeros((number_of,), jnp.int32).at[ranking[jnp.where(places < fixed, places, passed)]].set(jnp.asarray(tallies, jnp.int32))

    tallies = jnp.where(number % 4 == 0, named(crowded, number // 4), named(common, number - number // 4 - 1))
    mixed = jax.random.permutation(jax.random.fold_in(own, 3), number_of)
    donor, taker = mixed[0:number_of // 2 * 2:2], mixed[1:number_of // 2 * 2:2]
    room = jnp.minimum(tallies[donor] - 1, reach - tallies[taker]) // 2
    room = jnp.where((donor == ranking[0]) | (taker == ranking[0]) | (tallies[taker] == 0), 0, jnp.maximum(room, 0))
    passed = jax.random.randint(jax.random.fold_in(own, 4), (number_of // 2,), 0, 1 << 20) % (room + 1)
    tallies = tallies.at[donor].add(-passed).at[taker].add(passed)
    members = jnp.searchsorted(jnp.cumsum(tallies), jnp.arange(rows * top), side="right").astype(jnp.int32)
    listing = members.reshape(top, rows).T
    listing = listing[jax.random.permutation(jax.random.fold_in(own, 1), rows)]
    rotation = jax.random.randint(jax.random.fold_in(own, 2), (rows, 1), 0, top)
    return jnp.take_along_axis(listing, (jnp.arange(top)[None, :] + rotation) % top, axis=1)


def load_shares(amount, total, bound, slope, full):
    weights = [(1 << 20) // math.isqrt(rank ** slope) + 1 for rank in range(1, amount + 1)]
    largest = bound if full else min(bound, max(-(-total // amount), total * weights[0] // sum(weights)))
    least = 1 if total - largest >= amount - 1 else 0
    counts, surplus = [largest] + [least] * (amount - 1), total - largest - least * (amount - 1)
    while surplus > 0:
        movable = [i for i in range(1, amount) if counts[i] < largest] or [i for i in range(1, amount) if counts[i] < bound]
        pool, left = sum([weights[i] for i in movable]), surplus
        for i in movable:
            addition = min(bound - counts[i], max(1, left * weights[i] // pool), surplus)
            counts[i] = counts[i] + addition
            surplus = surplus - addition
    return np.array(counts)


def normal_values(own_key, shape, deviation, bound, pieces=(), kind=jnp.bfloat16):
    result = jax.random.normal(own_key, shape, jnp.float32) * deviation
    if len(pieces) > 0:
        result = levels(own_key, shape, pieces, -0.22, 0.18) * result
    return jnp.clip(result, min=-bound, max=bound).astype(kind)


def setup_inputs(seed: int = 0, part: int = 0) -> dict:
    splits = jax.random.split(jax.random.key(seed), 15)
    own_keys = jax.random.split(jax.random.fold_in(splits[14], part), 15)
    queries = normal_values(own_keys[0], (TOKENS, HEADS * QK_HEAD), 1.0, 6.0, ((0, 4), (1, 4)))
    keys = normal_values(own_keys[1], (TOKENS, HEADS * QK_HEAD), 1.0, 6.0, ((0, 4), (1, 4)))
    values = normal_values(own_keys[2], (TOKENS, HEADS * V_HEAD), 1.0, 6.0, ((0, 4), (1, 4)))
    in_gate = draw_in_gate(jax.random.fold_in(jax.random.fold_in(splits[14], part), 71), part)
    forget_gate = draw_forget_gate(jax.random.fold_in(jax.random.fold_in(splits[14], part), 71), part)
    head_gain = jnp.clip(1.0 + 0.18 * jax.random.normal(splits[5], (HEADS * V_HEAD,), jnp.float32), 0.1, 1.9)
    out_weight = normal_values(splits[6], (HEADS * V_HEAD, D), (HEADS * V_HEAD) ** -0.5, 0.125, ((0, 4),))
    resid = normal_values(own_keys[7], (TOKENS, D), 1.0, 6.0, ((0, 16),))
    norm_gain = jnp.clip(1.0 + 0.18 * jax.random.normal(splits[8], (D,), jnp.float32), 0.1, 1.9)
    expert_ids_keys = jax.random.split(jax.random.fold_in(own_keys[9], 1), TOKENS // TOK_SHARD)
    expert_ids_turns = jax.random.permutation(jax.random.fold_in(own_keys[9], 3), TOKENS // TOK_SHARD)
    expert_ids = jax.vmap(lambda own, number: routed_block(jax.random.fold_in(own_keys[9], 2), own, number, TOK_SHARD, EXPERTS, TOPK, CAP, 2))(expert_ids_keys, expert_ids_turns).reshape((TOKENS, TOPK))
    expert_mix = jnp.clip(jnp.exp(math.log(1.0) - 1.3862944 * jax.random.uniform(own_keys[10], (TOKENS, TOPK), jnp.float32) ** levels(own_keys[10], (TOKENS, TOPK), ((0, 16),), -0.2, 0.2)), 0.25, 1.0)
    gate_weight = normal_values(splits[11], (EXPERTS, D, FF), D ** -0.5, 0.125, ((0, 16),))
    up_weight = normal_values(splits[12], (EXPERTS, D, FF), D ** -0.5, 0.125, ((0, 16),))
    down_weight = normal_values(splits[13], (EXPERTS, FF, D), FF ** -0.5, 0.25, ((0, 16),))
    return dict(queries=queries, keys=keys, values=values, in_gate=in_gate, forget_gate=forget_gate, head_gain=head_gain, out_weight=out_weight, resid=resid, norm_gain=norm_gain, expert_ids=expert_ids, expert_mix=expert_mix, gate_weight=gate_weight, up_weight=up_weight, down_weight=down_weight)


EPSILON = 1e-06

def head_cell(packed):
    query_heads, keys_h, values_h, in_h, forget_h, gain_h = packed
    count = query_heads.shape[0] // BLOCK
    query_tiles = query_heads.reshape(count, BLOCK, QK_HEAD).astype(jnp.float32)
    key_blocks = keys_h.reshape(count, BLOCK, QK_HEAD).astype(jnp.float32)
    value_tiles = values_h.reshape(count, BLOCK, V_HEAD).astype(jnp.float32)
    in_blocks = in_h.reshape(count, BLOCK)
    log_forget = jax.nn.log_sigmoid(forget_h).reshape(count, BLOCK)
    cumulative = jnp.cumsum(log_forget, axis=1)
    totals = cumulative[:, -1]
    to_end = totals[:, None] - cumulative + in_blocks
    end_max = lax.optimization_barrier(jnp.max(to_end, axis=1))
    key_weighted = (key_blocks * jnp.exp(to_end - end_max[:, None])[:, :, None]).astype(jnp.bfloat16)
    key_forget_weighted = lax.optimization_barrier(key_weighted).astype(jnp.float32)
    state_per_block = jnp.einsum('foj,fop->fjp', value_tiles, key_forget_weighted)

    def advance(carry, input_rows):
        state, stab = carry
        total, bstate, bmax = input_rows
        new_stab = jnp.maximum(total + stab, bmax)
        keep = jnp.exp(total + stab - new_stab)
        added = jnp.exp(bmax - new_stab)
        return ((keep * state + added * bstate, new_stab), (state, stab))
    init = (jnp.zeros((V_HEAD, QK_HEAD), jnp.float32), jnp.zeros((), jnp.float32))
    _, (prev_state, prev_stab) = lax.scan(advance, init, (totals, state_per_block, end_max))
    scale = QK_HEAD ** (-0.5)
    scores = jnp.einsum('ctd,csd->cts', query_tiles, key_blocks) * scale
    causal = jnp.tril(jnp.ones((BLOCK, BLOCK), dtype=bool))
    gaps = cumulative[:, :, None] - cumulative[:, None, :] + in_blocks[:, None, :]
    gaps = jnp.where(causal, gaps, -jnp.inf)
    row_max = lax.optimization_barrier(jnp.max(gaps, axis=2))
    weights = scores * jnp.exp(gaps - row_max[:, :, None])
    rounded = lax.optimization_barrier(weights.astype(jnp.bfloat16)).astype(jnp.float32)
    local_num = jnp.einsum('cts,csv->ctv', rounded, value_tiles)
    inter = cumulative + prev_stab[:, None]
    stab = jnp.maximum(inter, row_max)
    own_scale = jnp.exp(row_max - stab)
    carried = jnp.exp(inter - stab)
    query_scaled = query_tiles * scale
    memory_readout = jnp.einsum('ctk,cvk->ctv', query_scaled, prev_state, precision=lax.Precision.HIGHEST)
    cell = own_scale[..., None] * local_num + carried[..., None] * memory_readout
    cell = cell.reshape(-1, V_HEAD)
    normed = cell * lax.rsqrt(lax.optimization_barrier(jnp.mean(cell * cell, axis=1, keepdims=True)) + EPSILON)
    return normed * gain_h

def reference(queries, keys, values, in_gate, forget_gate, head_gain, out_weight, resid, norm_gain, expert_ids, expert_mix, gate_weight, up_weight, down_weight):
    tokens = queries.shape[0]
    packed = (queries.reshape(tokens, HEADS, QK_HEAD).transpose(1, 0, 2), keys.reshape(tokens, HEADS, QK_HEAD).transpose(1, 0, 2), values.reshape(tokens, HEADS, V_HEAD).transpose(1, 0, 2), in_gate, forget_gate, head_gain.reshape(HEADS, V_HEAD))
    cells = lax.map(head_cell, packed)
    mixed = cells.transpose(1, 0, 2).reshape(tokens, HEADS * V_HEAD).astype(jnp.bfloat16)
    group = HEADS * V_HEAD // N_TP
    proj = jnp.zeros((tokens, D), jnp.float32)
    for group_no in range(N_TP):
        partial_sum = jnp.dot(mixed[:, group_no * group:(group_no + 1) * group], out_weight[group_no * group:(group_no + 1) * group], preferred_element_type=jnp.float32)
        proj = proj + lax.optimization_barrier(partial_sum.astype(jnp.bfloat16)).astype(jnp.float32)
    mid = (resid.astype(jnp.float32) + proj).astype(jnp.bfloat16)
    mid_f = mid.astype(jnp.float32)
    normed = (mid_f * lax.rsqrt(lax.optimization_barrier(jnp.mean(mid_f * mid_f, axis=1, keepdims=True)) + EPSILON) * norm_gain).astype(jnp.bfloat16)
    share = expert_mix / lax.optimization_barrier(jnp.sum(expert_mix, axis=1, keepdims=True))
    flat_ids = expert_ids.reshape(-1)
    flat_share = share.reshape(-1)
    count_all = flat_ids.shape[0]
    order = jnp.argsort(flat_ids, stable=True).astype(jnp.int32)
    loads = jax.ops.segment_sum(jnp.ones_like(flat_ids), flat_ids, num_segments=EXPERTS).astype(jnp.int32)
    starts = (jnp.cumsum(loads) - loads).astype(jnp.int32)
    room = EXPERTS * CAP

    def run_expert(total, expert):
        offsets = jnp.arange(room, dtype=jnp.int32)
        picks = order[jnp.minimum(starts[expert] + offsets, count_all - 1)]
        valid = offsets < loads[expert]
        token_rows = (picks // TOPK).astype(jnp.int32)
        rows = normed[token_rows]
        gate = jnp.dot(rows, gate_weight[expert], preferred_element_type=jnp.float32)
        upper = jnp.dot(rows, up_weight[expert], preferred_element_type=jnp.float32)
        hidden = (jax.nn.silu(gate) * upper).astype(jnp.bfloat16)
        output = jnp.dot(hidden, down_weight[expert], preferred_element_type=jnp.float32).astype(jnp.bfloat16)
        weight = jnp.where(valid, flat_share[picks], 0.0)
        return (total.at[token_rows].add(weight[:, None] * output.astype(jnp.float32)), None)
    total, _ = lax.scan(run_expert, jnp.zeros((tokens, D), jnp.float32), jnp.arange(EXPERTS, dtype=jnp.int32))
    return (mid_f + total).astype(jnp.bfloat16)
```

```python
import functools

import jax
import jax.numpy as jnp
from jax import lax
from jax.experimental import pallas as pl
from jax.experimental.pallas import tpu as pltpu
from jax.sharding import PartitionSpec as P

QK_HEAD = 128
V_HEAD = 256
BLOCK = 128
TOPK = 2
CAP_FACTOR = 4


EPSILON = 1e-06
VERY_LOW = -1e30


def entering(x, axis, combine, identity):
    count, position = (lax.axis_size(axis), lax.axis_index(axis))
    everything = jax.tree.map(lambda part: lax.all_gather(part, axis), x)
    start = jax.tree.map(
        lambda part, zero: jnp.broadcast_to(jnp.asarray(zero, part.dtype), part.shape), x, identity
    )

    def hop(k, before):
        reached = k < position
        new = combine(before, jax.tree.map(lambda part: part[k], everything))
        return jax.tree.map(lambda a, b: jnp.where(reached, a, b), new, before)

    return lax.fori_loop(0, count, hop, start)


def join_states(before_part, after_part):
    before_total, before_state, before_stab = before_part
    after_total, after_state, after_stab = after_part
    stab = jnp.maximum(before_stab + after_total, after_stab)
    keep = jnp.exp(before_stab + after_total - stab)
    added = jnp.exp(after_stab - stab)
    return (
        before_total + after_total,
        before_state * keep[:, None, None] + after_state * added[:, None, None],
        stab,
    )


def expert_ffn(arrived, gate_weight, up_weight, down_weight):
    width = arrived.shape[-1]
    flat = arrived.reshape(-1, width)
    gate = jnp.dot(flat, gate_weight[0], preferred_element_type=jnp.float32)
    upper = jnp.dot(flat, up_weight[0], preferred_element_type=jnp.float32)
    hidden = (jax.nn.silu(gate) * upper).astype(jnp.bfloat16)
    output = jnp.dot(hidden, down_weight[0], preferred_element_type=jnp.float32).astype(
        jnp.bfloat16
    )
    return output.reshape(arrived.shape)


MESH = pl.DeviceIdType.MESH
LANES = 128
PAIR = 2
VMEM_BUDGET = 40 * 2**20


def flip(index, bits, count):
    out, step = index, 1
    while step < count:
        if bits & step:
            out = out + step * (1 - 2 * ((index // step) % 2))
        step *= 2
    return out


def moe_kernel(
    n_sp,
    piece_ref,
    mid_ref,
    gate_ref,
    up_ref,
    down_ref,
    out_ref,
    buf,
    hid,
    mine,
    sib_out,
    sib_in,
    x_out,
    x_in,
    z_out,
    z_in,
    keep,
    ag_recv,
    ag_z,
    ag_x,
    ag_s,
    s_send,
    s_recv,
    x_send,
    x_recv,
    z_send,
    z_recv,
    own_sem,
):
    rows, width = mid_ref.shape
    ff = gate_ref.shape[1]
    z = lax.axis_index("sp")
    t = lax.axis_index("tp")
    x, c = t // PAIR, t % PAIR
    ox, oc = 1 - x, 1 - c
    expert = z * lax.axis_size("tp") + t
    experts = n_sp * lax.axis_size("tp")
    sib = {"tp": x * PAIR + oc}
    part = {"tp": ox * PAIR + c}

    def line(d):
        return {"sp": flip(z, d, n_sp)}

    barrier = pltpu.get_barrier_semaphore()
    peers = [sib, part] + [line(d) for d in range(1, n_sp)]
    for peer in peers:
        pl.semaphore_signal(barrier, inc=1, device_id=peer, device_id_type=MESH)
    pl.semaphore_wait(barrier, len(peers))

    def remote(src, dst, send, recv, peer):
        return pltpu.make_async_remote_copy(
            src_ref=src, dst_ref=dst, send_sem=send, recv_sem=recv, device_id=peer, device_id_type=MESH
        )

    def slot(zz, xx, cc):
        return buf.at[zz * PAIR + xx, cc]

    def arrived(zz, xx, cc):
        ref = slot(zz, xx, cc)
        sem = ag_recv.at[zz * PAIR + xx, cc]
        pltpu.make_async_copy(ref, ref, sem).wait()

    def send_ag(src, zz, xx, sem, peer):
        copy = remote(src, slot(zz, xx, c), sem, ag_recv.at[zz * PAIR + xx, c], peer)
        copy.start()
        return copy

    pending = []
    own = pltpu.make_async_copy(piece_ref, slot(z, x, c), own_sem)
    own.start()
    pending.append(send_ag(piece_ref, z, x, ag_x.at[0], part))
    for d in range(1, n_sp):
        pending.append(send_ag(piece_ref, z, x, ag_z.at[d], line(d)))
    pending.append(send_ag(piece_ref, z, x, ag_s.at[0, 0], sib))
    own.wait()

    def forward(d):
        zz = flip(z, d, n_sp)
        arrived(zz, x, c)
        pending.append(send_ag(slot(zz, x, c), zz, x, ag_x.at[d], part))
        pending.append(send_ag(slot(zz, x, c), zz, x, ag_s.at[d, 0], sib))

    lane = lax.broadcasted_iota(jnp.int32, (rows, LANES), 1)

    def compute(pair):
        for i in range(0, ff, 256):
            a = buf[pair, :, :, :width].reshape(PAIR * rows, width)
            g = jnp.dot(a, gate_ref[:, i : i + 256], preferred_element_type=jnp.float32)
            u = jnp.dot(a, up_ref[:, i : i + 256], preferred_element_type=jnp.float32)
            hid[:, i : i + 256] = (jax.nn.silu(g) * u).astype(jnp.bfloat16)

    def weight(pair, cc):
        w = buf[pair, cc, :, width:].astype(jnp.float32)
        chosen = (lane == expert) | (lane == expert + experts)
        return jnp.sum(jnp.where(chosen, w, 0.0), axis=1, keepdims=True)

    def down(pair):
        w_mine, w_sib = weight(pair, c), weight(pair, oc)
        h_mine = hid[pl.ds(pl.multiple_of(c * rows, rows), rows), :]
        h_sib = hid[pl.ds(pl.multiple_of(oc * rows, rows), rows), :]
        both = jnp.concatenate([h_mine, h_sib], axis=0)
        for j in range(0, width, 512):
            o = jnp.dot(both, down_ref[:, j : j + 512], preferred_element_type=jnp.float32)
            mine[:, j : j + 512] = o[:rows] * w_mine
            sib_out[pair, :, j : j + 512] = (o[rows:] * w_sib).astype(jnp.bfloat16)

    def exchange(pair):
        copy = remote(sib_out.at[pair], sib_in.at[pair], s_send.at[pair], s_recv.at[pair], sib)
        copy.start()
        copy.wait()

    def step_own(d):
        zz = flip(z, d, n_sp)
        arrived(zz, x, oc)
        pair = zz * PAIR + x
        compute(pair)
        down(pair)
        exchange(pair)
        keep[d] = mine[...] + sib_in[pair].astype(jnp.float32)

    def step_other(d):
        zz = flip(z, d, n_sp)
        arrived(zz, ox, c)
        copy = send_ag(slot(zz, ox, c), zz, ox, ag_s.at[d, 1], sib)
        pending.append(copy)
        arrived(zz, ox, oc)
        pair = zz * PAIR + ox
        compute(pair)
        down(pair)
        exchange(pair)
        x_out[d] = (mine[...] + sib_in[pair].astype(jnp.float32)).astype(jnp.bfloat16)
        copy = remote(x_out.at[d], x_in.at[d], x_send.at[d], x_recv.at[d], part)
        copy.start()
        return copy

    def finish(d, copy):
        copy.wait()
        total = keep[d] + x_in[d].astype(jnp.float32)
        if d == 0:
            keep[0] = total
            return
        z_out[d] = total.astype(jnp.bfloat16)
        back = remote(z_out.at[d], z_in.at[d], z_send.at[d], z_recv.at[d], line(d))
        back.start()
        returns.append((d, back))

    returns, crossed = [], []
    for d in range(n_sp):
        step_own(d)
        if d + 1 < n_sp:
            forward(d + 1)
        crossed.append(step_other(d))
        if d > 0:
            finish(d - 1, crossed[d - 1])
    finish(n_sp - 1, crossed[n_sp - 1])
    total = keep[0]
    for d, back in returns:
        back.wait()
        total = total + z_in[d].astype(jnp.float32)
    out_ref[...] = (mid_ref[...].astype(jnp.float32) + total).astype(jnp.bfloat16)
    for copy in pending:
        copy.wait_send()


def moe_bytes(rows, width, n_sp, n_tp):
    return n_sp * n_tp * rows * width * 2 * 3


def moe(piece, mid, gate_weight, up_weight, down_weight):
    n_sp = lax.axis_size("sp")
    rows, width = mid.shape
    pairs = n_sp * PAIR
    ff = gate_weight.shape[-1]
    bf, f32 = jnp.bfloat16, jnp.float32
    dma = pltpu.SemaphoreType.DMA
    return pl.pallas_call(
        functools.partial(moe_kernel, n_sp),
        out_shape=jax.ShapeDtypeStruct((rows, width), bf),
        in_specs=[pl.BlockSpec(memory_space=pltpu.VMEM)] * 5,
        out_specs=pl.BlockSpec(memory_space=pltpu.VMEM),
        scratch_shapes=[
            pltpu.VMEM((pairs, PAIR, rows, piece.shape[1]), bf),
            pltpu.VMEM((PAIR * rows, ff), bf),
            pltpu.VMEM((rows, width), f32),
            pltpu.VMEM((pairs, rows, width), bf),
            pltpu.VMEM((pairs, rows, width), bf),
            pltpu.VMEM((n_sp, rows, width), bf),
            pltpu.VMEM((n_sp, rows, width), bf),
            pltpu.VMEM((n_sp, rows, width), bf),
            pltpu.VMEM((n_sp, rows, width), bf),
            pltpu.VMEM((n_sp, rows, width), f32),
            dma((pairs, PAIR)),
            dma((n_sp,)),
            dma((n_sp,)),
            dma((n_sp, PAIR)),
            dma((pairs,)),
            dma((pairs,)),
            dma((n_sp,)),
            dma((n_sp,)),
            dma((n_sp,)),
            dma((n_sp,)),
            dma,
        ],
        compiler_params=pltpu.CompilerParams(
            collective_id=3, has_side_effects=True, vmem_limit_bytes=60 * 2**20
        ),
        name="moe",
    )(piece, mid, gate_weight, up_weight, down_weight)


def row_weights(expert_ids, expert_mix, experts):
    share = expert_mix / jnp.sum(expert_mix, axis=1, keepdims=True)
    names = jnp.arange(experts, dtype=jnp.int32)
    dense = jnp.sum(
        jnp.where(expert_ids[:, :, None] == names[None, None, :], share[:, :, None], 0.0), axis=1
    )
    high = lax.reduce_precision(dense, 8, 7)
    low = dense - high
    both = jnp.concatenate([high, low], axis=1).astype(jnp.bfloat16)
    return jnp.pad(both, ((0, 0), (0, -both.shape[1] % LANES)))


def per_device(
    queries,
    keys,
    values,
    in_gate,
    forget_gate,
    head_gain,
    out_weight,
    resid,
    norm_gain,
    expert_ids,
    expert_mix,
    gate_weight,
    up_weight,
    down_weight,
):
    tokens = queries.shape[0]
    heads = in_gate.shape[0]
    count = tokens // BLOCK
    scale = QK_HEAD ** (-0.5)
    query_tiles = queries.reshape(count, BLOCK, heads, QK_HEAD)
    key_blocks = keys.reshape(count, BLOCK, heads, QK_HEAD)
    value_tiles = values.reshape(count, BLOCK, heads, V_HEAD)
    in_blocks = in_gate.reshape(heads, count, BLOCK)
    cumulative = jnp.cumsum(jax.nn.log_sigmoid(forget_gate).reshape(heads, count, BLOCK), axis=2)
    totals = cumulative[:, :, -1]
    to_end = totals[:, :, None] - cumulative + in_blocks
    end_max = jnp.max(to_end, axis=2)
    end_weight = jnp.exp(to_end - end_max[:, :, None]).transpose(1, 2, 0)
    key_weighted = (key_blocks * end_weight[..., None]).astype(jnp.bfloat16)
    state_per_block = jnp.einsum(
        "clhv,clhk->hcvk", value_tiles, key_weighted, preferred_element_type=jnp.float32
    )
    summary = (totals[:, 0], state_per_block[:, 0], end_max[:, 0])
    for block_no in range(1, count):
        summary = join_states(
            summary, (totals[:, block_no], state_per_block[:, block_no], end_max[:, block_no])
        )
    identity = (
        jnp.zeros_like(summary[0]),
        jnp.zeros_like(summary[1]),
        jnp.full_like(summary[2], VERY_LOW),
    )
    prefix = entering(summary, "sp", join_states, identity)
    enter_stab = jnp.maximum(prefix[0], prefix[2])
    factor = jnp.exp(prefix[2] - enter_stab)
    enter_state = prefix[1] * factor[:, None, None]
    state, stab = (enter_state, enter_stab)
    state_list, stab_list = ([], [])
    for block_no in range(count):
        state_list.append(state)
        stab_list.append(stab)
        new_stab = jnp.maximum(totals[:, block_no] + stab, end_max[:, block_no])
        keep = jnp.exp(totals[:, block_no] + stab - new_stab)
        added = jnp.exp(end_max[:, block_no] - new_stab)
        state = state * keep[:, None, None] + state_per_block[:, block_no] * added[:, None, None]
        stab = new_stab
    prev_state = jnp.stack(state_list, axis=1)
    prev_stab = jnp.stack(stab_list, axis=1)
    scores = (
        jnp.einsum("cthd,cshd->hcts", query_tiles, key_blocks, preferred_element_type=jnp.float32)
        * scale
    )
    causal = jnp.tril(jnp.ones((BLOCK, BLOCK), dtype=bool))
    gaps = cumulative[..., :, None] - cumulative[..., None, :] + in_blocks[..., None, :]
    gaps = jnp.where(causal, gaps, -jnp.inf)
    row_max = jnp.max(gaps, axis=3)
    weights = scores * jnp.exp(gaps - row_max[..., None])
    rounded = weights.astype(jnp.bfloat16)
    local_num = jnp.einsum(
        "hcts,cshv->hctv", rounded, value_tiles, preferred_element_type=jnp.float32
    )
    inter = cumulative + prev_stab[..., None]
    stab_t = jnp.maximum(inter, row_max)
    own_scale = jnp.exp(row_max - stab_t)
    carried = jnp.exp(inter - stab_t)
    query_scaled = query_tiles.astype(jnp.float32) * scale
    memory_readout = jnp.einsum(
        "cthk,hcvk->hctv", query_scaled, prev_state, precision=lax.Precision.HIGHEST
    )
    cell = own_scale[..., None] * local_num + carried[..., None] * memory_readout
    cell = cell * lax.rsqrt(jnp.mean(cell * cell, axis=3, keepdims=True) + EPSILON)
    cell = cell * head_gain.reshape(heads, 1, 1, V_HEAD)
    mixed = cell.transpose(1, 2, 0, 3).reshape(tokens, heads * V_HEAD).astype(jnp.bfloat16)
    shard = tokens // lax.axis_size("tp")
    proj = lax.psum_scatter(
        jnp.dot(mixed, out_weight, preferred_element_type=jnp.float32).astype(jnp.bfloat16),
        "tp",
        scatter_dimension=0,
        tiled=True,
    ).astype(jnp.float32)
    mid_f = (resid.astype(jnp.float32) + proj).astype(jnp.bfloat16).astype(jnp.float32)
    normed = (
        mid_f * lax.rsqrt(jnp.mean(mid_f * mid_f, axis=1, keepdims=True) + EPSILON) * norm_gain
    ).astype(jnp.bfloat16)
    width = normed.shape[1]
    expert_group = lax.axis_size("sp") * lax.axis_size("tp")
    n_sp, n_tp = lax.axis_size("sp"), lax.axis_size("tp")
    if n_tp == PAIR * PAIR and moe_bytes(shard, width, n_sp, n_tp) <= VMEM_BUDGET:
        piece = jnp.concatenate([normed, row_weights(expert_ids, expert_mix, expert_group)], axis=1)
        return moe(
            piece, mid_f.astype(jnp.bfloat16), gate_weight[0], up_weight[0], down_weight[0]
        )
    assigns = expert_ids.reshape(-1)
    assign_count = assigns.shape[0]
    slots_each = CAP_FACTOR * assign_count // expert_group
    one_hot = (assigns[:, None] == jnp.arange(expert_group, dtype=jnp.int32)[None, :]).astype(
        jnp.bfloat16
    )
    earlier_mask = jnp.tril(jnp.ones((assign_count, assign_count), jnp.bfloat16), -1)
    counts_before = jnp.dot(earlier_mask, one_hot, preferred_element_type=jnp.float32)
    slot = jnp.sum(counts_before * one_hot.astype(jnp.float32), axis=1).astype(jnp.int32)
    target = assigns * slots_each + slot
    filler = (
        jnp.full((expert_group * slots_each,), -1, jnp.int32)
        .at[target]
        .set(jnp.arange(assign_count, dtype=jnp.int32))
    )
    rows_from = jnp.maximum(filler, 0) // TOPK
    outgoing = jnp.where((filler >= 0)[:, None], normed[rows_from], jnp.zeros((), jnp.bfloat16))
    outgoing = outgoing.reshape(expert_group, slots_each, width)
    served = expert_ffn(
        lax.all_to_all(outgoing, ("sp", "tp"), split_axis=0, concat_axis=0, tiled=True),
        gate_weight,
        up_weight,
        down_weight,
    )
    returned = lax.all_to_all(served, ("sp", "tp"), split_axis=0, concat_axis=0, tiled=True)
    picked = returned.reshape(expert_group * slots_each, width)[target]
    picked = picked.reshape(shard, TOPK, width).astype(jnp.float32)
    share = expert_mix / jnp.sum(expert_mix, axis=1, keepdims=True)
    total = jnp.sum(share[:, :, None] * picked, axis=1)
    return (mid_f + total).astype(jnp.bfloat16)


def solution(mesh):
    in_specs = (
        P(("grp", "sp"), "tp"),
        P(("grp", "sp"), "tp"),
        P(("grp", "sp"), "tp"),
        P("tp", ("grp", "sp")),
        P("tp", ("grp", "sp")),
        P("tp"),
        P("tp", None),
        P(("grp", "sp", "tp"), None),
        P(),
        P(("grp", "sp", "tp"), None),
        P(("grp", "sp", "tp"), None),
        P(("sp", "tp"), None, None),
        P(("sp", "tp"), None, None),
        P(("sp", "tp"), None, None),
    )
    out_specs = P(("grp", "sp", "tp"), None)
    return jax.shard_map(
        per_device, mesh=mesh, in_specs=in_specs, out_specs=out_specs, check_vma=False
    )
```
